32 devices in a mesh: sp: 8 (over z, y), dp: 4 (over x, core).
Axes of the slice: x: 2, y: 2, z: 4, core: 2. Of those that a mesh axis runs over, the one named last changes fastest.
Arguments:
- residual: bfloat16 [4, 1024, 2048], P('dp', 'sp'), may hold values from -6 to 6
- head_input: bfloat16 [4, 1024, 2048], P('dp', 'sp'), may hold values from -6 to 6
- gate_input: bfloat16 [4, 1024, 2048], P('dp', 'sp'), may hold values from -6 to 6
- b_input: bfloat16 [4, 1024, 1024], P('dp', 'sp'), may hold values from -6 to 6
- c_input: bfloat16 [4, 1024, 1024], P('dp', 'sp'), may hold values from -6 to 6
- step_input: bfloat16 [4, 1024, 32], P('dp', 'sp'), may hold values from -4.8 to 4.8
- conv_weight: bfloat16 [4, 2048], replicated, may hold values from -3 to 3
- conv_b_weight: bfloat16 [4, 1024], replicated, may hold values from -3 to 3
- conv_c_weight: bfloat16 [4, 1024], replicated, may hold values from -3 to 3
- step_bias: float32 [32], replicated, may hold values from -1 to 1
- decay_log: float32 [32], replicated, may hold values from -9.92 to -2.99
- skip: float32 [32], replicated, may hold values from 0.5 to 1.5
- norm_gain: float32 [2048], replicated, may hold values from 0.1 to 1.9
- out_weight: bfloat16 [2048, 2048], P('dp'), may hold values from -0.125 to 0.125
- ffn_gain: float32 [2048], replicated, may hold values from 0.1 to 1.9
- shared_gate: bfloat16 [2048, 512], replicated, may hold values from -0.125 to 0.125
- shared_up: bfloat16 [2048, 512], replicated, may hold values from -0.125 to 0.125
- shared_down: bfloat16 [512, 2048], replicated, may hold values from -0.25 to 0.25
- expert_gate: bfloat16 [32, 2048, 512], P(('sp', 'dp')), may hold values from -0.125 to 0.125
- expert_up: bfloat16 [32, 2048, 512], P(('sp', 'dp')), may hold values from -0.125 to 0.125
- expert_down: bfloat16 [32, 512, 2048], P(('sp', 'dp')), may hold values from -0.25 to 0.25
- routes: int32 [4, 1024, 2], P('dp', 'sp'), may hold values from 0 to 31, all different within a row; in each aligned block of 128 rows (0 to 127, 128 to 255, ..., all dimensions but the last counted through in order) at most 16 rows name the same one
- route_weights: float32 [4, 1024, 2], P('dp', 'sp'), may hold values from 0.25 to 1.25
Outputs:
- layer_out: bfloat16 [4, 1024, 2048], P('dp', 'sp')
The draws below stay inside these ranges and needn't reach their ends.
Inputs may be any that keep to these rules, and one draw needn't show every extreme that they name: `routes`: each token names 2 different experts; among the rows of one device no expert is named more than 16 times, a bound that some block reaches.
All inputs are finite; a program needn't handle non-finite values.
Results may differ from the reference program's by a relative error of at most 0.015.
Values may be sent and summed in bfloat16 or wider, within the bound.
A program may use at most 128 MiB of HBM per device.

```python
import math
import jax
import jax.numpy as jnp
import numpy as np
from jax import lax

D = 2048
HEADS = 32
HEAD_DIM = 64
GROUPS = 8
STATE = 128
CONV_K = 4
BLOCK = 128
EXPERT_FF = 512
SHARED_FF = 512
TOP_K = 2
TOK_DEV = 128
INNER = 2048
SEQS = 4
LENGTH = 1024
EXPERTS = 32
CAP = 16
N_SP = 8
N_DP = 4


def draw_decay_log(key, part):
    first, second, third = jax.random.split(key, 3)
    share = 0.5
    quick = jax.random.uniform(first, (HEADS,), jnp.float32) < share
    slow = jax.random.uniform(second, (HEADS,), jnp.float32, math.log(5e-05), math.log(0.0002))
    fast = jax.random.uniform(third, (HEADS,), jnp.float32, math.log(0.015), math.log(0.05))
    return jnp.where(quick, fast, slow).astype(jnp.float32)


def draw_step_input(key, part):
    first, second = jax.random.split(key)
    count = LENGTH // TOK_DEV
    offset = jax.random.uniform(second, (SEQS, count, 1, HEADS), jnp.float32, -1.2, 1.2)
    noise = jnp.clip(jax.random.normal(first, (SEQS, count, TOK_DEV, HEADS), jnp.float32) * 0.6, -3.5, 3.5)
    return (offset + noise).reshape(SEQS, LENGTH, HEADS).astype(jnp.bfloat16)


def shard_levels(own_key, shape, pieces, least, largest):
    factor_of = 1.0
    for dim, blocks in pieces:
        steps = jax.random.uniform(jax.random.fold_in(jax.random.fold_in(own_key, 6), dim), (blocks,), jnp.float32, least / len(pieces), largest / len(pieces))
        factor_of = factor_of * jnp.repeat(jnp.exp(steps), shape[dim] // blocks).reshape((-1,) + (1,) * (len(shape) - 1 - dim))
    return factor_of


def routed_block(stream_key, own, number, rows, count, top, limit, slope):
    sequence = jax.random.permutation(stream_key, count)
    crowded, ordinary = load_shares(count, rows * top, limit, slope, True), load_shares(count, rows * top, limit, slope, False)
    places = jnp.arange(count)

    def named(lengths, rotation):
        used = int((lengths > 0).sum())
        fixed = max(1, used // 4)
        shifted = fixed + (places - fixed + rotation * (used - fixed)) % max(1, count - fixed)
        return jnp.zeros((count,), jnp.int32).at[sequence[jnp.where(places < fixed, places, shifted)]].set(jnp.asarray(lengths, jnp.int32))

    lengths = jnp.where(number % 4 == 0, named(crowded, number // 4), named(ordinary, number - number // 4 - 1))
    mixed = jax.random.permutation(jax.random.fold_in(own, 3), count)
    donor, receiver = mixed[0:count // 2 * 2:2], mixed[1:count // 2 * 2:2]
    room = jnp.minimum(lengths[donor] - 1, limit - lengths[receiver]) // 2
    room = jnp.where((donor == sequence[0]) | (receiver == sequence[0]) | (lengths[receiver] == 0), 0, jnp.maximum(room, 0))
    shifted = jax.random.randint(jax.random.fold_in(own, 4), (count // 2,), 0, 1 << 20) % (room + 1)
    lengths = lengths.at[donor].add(-shifted).at[receiver].add(shifted)
    labels = jnp.searchsorted(jnp.cumsum(lengths), jnp.arange(rows * top), side="right").astype(jnp.int32)
    listing = labels.reshape(top, rows).T
    listing = listing[jax.random.permutation(jax.random.fold_in(own, 1), rows)]
    rotation = jax.random.randint(jax.random.fold_in(own, 2), (rows, 1), 0, top)
    return jnp.take_along_axis(listing, (jnp.arange(top)[None, :] + rotation) % top, axis=1)


def load_shares(count, total, reach, slope, full):
    loads = [(1 << 20) // math.isqrt(rank ** slope) + 1 for rank in range(1, count + 1)]
    largest = reach if full else min(reach, max(-(-total // count), total * loads[0] // sum(loads)))
    least = 1 if total - largest >= count - 1 else 0
    given, rest = [largest] + [least] * (count - 1), total - largest - least * (count - 1)
    while rest > 0:
        movable = [i for i in range(1, count) if given[i] < largest] or [i for i in range(1, count) if given[i] < reach]
        pool, budget = sum([loads[i] for i in movable]), rest
        for i in movable:
            extra = min(reach - given[i], max(1, budget * loads[i] // pool), rest)
            given[i] = given[i] + extra
            rest = rest - extra
    return np.array(given)


def scatter_about(own_key, extent, scale, bound, pieces=(), kind=jnp.bfloat16):
    values = scale * jax.random.normal(own_key, extent, jnp.float32)
    if pieces:
        values = values * shard_levels(own_key, extent, pieces, -0.22, 0.18)
    return jnp.clip(values, -bound, bound).astype(kind)


def setup_inputs(seed: int = 0) -> dict:
    keys = jax.random.split(jax.random.key(seed), 24)
    residual = scatter_about(keys[0], (SEQS, LENGTH, D), 1.0, 6.0, ((0, 4), (1, 8)))
    head_input = scatter_about(keys[1], (SEQS, LENGTH, INNER), 1.0, 6.0, ((0, 4), (1, 8)))
    gate_input = scatter_about(keys[2], (SEQS, LENGTH, INNER), 1.0, 6.0, ((0, 4), (1, 8)))
    b_input = scatter_about(keys[3], (SEQS, LENGTH, GROUPS * STATE), 1.0, 6.0, ((0, 4), (1, 8)))
    c_input = scatter_about(keys[4], (SEQS, LENGTH, GROUPS * STATE), 1.0, 6.0, ((0, 4), (1, 8)))
    step_input = draw_step_input(jax.random.fold_in(keys[23], 71), 0)
    conv_weight = scatter_about(keys[6], (CONV_K, INNER), 0.5, 3.0)
    conv_b_weight = scatter_about(keys[7], (CONV_K, GROUPS * STATE), 0.5, 3.0)
    conv_c_weight = scatter_about(keys[8], (CONV_K, GROUPS * STATE), 0.5, 3.0)
    step_bias = jnp.clip(jax.random.uniform(keys[9], (HEADS,), jnp.float32, -1.0, 1.0), -1.0, 1.0)
    decay_log = draw_decay_log(jax.random.fold_in(keys[23], 71), 0)
    skip = jnp.clip(jax.random.uniform(keys[11], (HEADS,), jnp.float32, 0.5, 1.5), 0.5, 1.5)
    norm_gain = jnp.clip(1.0 + 0.18 * jax.random.normal(keys[12], (INNER,), jnp.float32), 0.1, 1.9)
    out_weight = scatter_about(keys[13], (INNER, D), INNER ** -0.5, 0.125, ((0, 4),))
    ffn_gain = jnp.clip(1.0 + 0.18 * jax.random.normal(keys[14], (D,), jnp.float32), 0.1, 1.9)
    shared_gate = scatter_about(keys[15], (D, SHARED_FF), D ** -0.5, 0.125)
    shared_up = scatter_about(keys[16], (D, SHARED_FF), D ** -0.5, 0.125)
    shared_down = scatter_about(keys[17], (SHARED_FF, D), SHARED_FF ** -0.5, 0.25)
    expert_gate = scatter_about(keys[18], (EXPERTS, D, EXPERT_FF), D ** -0.5, 0.125, ((0, 32),))
    expert_up = scatter_about(keys[19], (EXPERTS, D, EXPERT_FF), D ** -0.5, 0.125, ((0, 32),))
    expert_down = scatter_about(keys[20], (EXPERTS, EXPERT_FF, D), EXPERT_FF ** -0.5, 0.25, ((0, 32),))
    routes_keys = jax.random.split(jax.random.fold_in(keys[21], 1), SEQS * LENGTH // TOK_DEV)
    routes_turns = jax.random.permutation(jax.random.fold_in(keys[21], 3), SEQS * LENGTH // TOK_DEV)
    routes = jax.vmap(lambda own, number: routed_block(jax.random.fold_in(keys[21], 2), own, number, TOK_DEV, EXPERTS, TOP_K, CAP, 2))(routes_keys, routes_turns).reshape((SEQS, LENGTH, TOP_K))
    route_weights = jnp.clip(0.25 + 1.0 * jax.random.uniform(keys[22], (SEQS, LENGTH, TOP_K), jnp.float32) ** shard_levels(keys[22], (SEQS, LENGTH, TOP_K), ((0, 4), (1, 8)), -0.2, 0.2), 0.25, 1.25)
    return {"residual": residual, "head_input": head_input, "gate_input": gate_input, "b_input": b_input, "c_input": c_input, "step_input": step_input, "conv_weight": conv_weight, "conv_b_weight": conv_b_weight, "conv_c_weight": conv_c_weight, "step_bias": step_bias, "decay_log": decay_log, "skip": skip, "norm_gain": norm_gain, "out_weight": out_weight, "ffn_gain": ffn_gain, "shared_gate": shared_gate, "shared_up": shared_up, "shared_down": shared_down, "expert_gate": expert_gate, "expert_up": expert_up, "expert_down": expert_down, "routes": routes, "route_weights": route_weights}


EPS = 1e-06
HIGH = lax.Precision.HIGHEST

def conv_silu(padded, weight, length):
    total = jnp.zeros((length, padded.shape[1]), jnp.float32)
    for tap in range(weight.shape[0]):
        total = total + padded[tap:tap + length].astype(jnp.float32) * weight[tap].astype(jnp.float32)
    return jax.nn.silu(total)

def block_scan(xs, step, rate, bmat, cmat, block, init):
    length, heads, width = xs.shape
    count = length // block
    logs = (step * rate[None, :]).reshape(count, block, heads)
    weighted = (xs * step[:, :, None]).reshape(count, block, heads, width)
    bb = bmat.reshape(count, block, heads, -1)
    cc = cmat.reshape(count, block, heads, -1)
    cum = jnp.cumsum(logs, axis=1)
    lower = jnp.tril(jnp.ones((block, block), dtype=bool))[None, :, :, None]
    diff = cum[:, :, None, :] - cum[:, None, :, :]
    decay = jnp.where(lower, jnp.exp(jnp.where(lower, diff, 0.0)), 0.0)
    scores = jnp.einsum('clhn,cshn->clsh', cc, bb, precision=HIGH) * decay
    inner = jnp.einsum('clsh,cshp->clhp', scores, weighted, precision=HIGH)
    to_end = jnp.exp(cum[:, -1:, :] - cum)
    states = jnp.einsum('cshn,cshp->chpn', bb * to_end[..., None], weighted, precision=HIGH)
    totals = jnp.exp(cum[:, -1, :])

    def advance(carry, item):
        fresh, factor = item
        return (carry * factor[:, None, None] + fresh, carry)
    last, before = lax.scan(advance, init, (states, totals))
    outer = jnp.einsum('clhn,chpn->clhp', cc * jnp.exp(cum)[..., None], before, precision=HIGH)
    return ((inner + outer).reshape(length, heads, width), last)

def reference(residual, head_input, gate_input, b_input, c_input, step_input, conv_weight, conv_b_weight, conv_c_weight, step_bias, decay_log, skip, norm_gain, out_weight, ffn_gain, shared_gate, shared_up, shared_down, expert_gate, expert_up, expert_down, routes, route_weights):
    taps = jnp.concatenate([conv_weight, conv_b_weight, conv_c_weight], axis=1)
    rate = -jnp.exp(decay_log)
    per_group = HEADS // GROUPS
    span = GROUPS * STATE

    def one_sequence(items):
        x_seq, b_seq, c_seq, s_seq, g_seq, r_seq = items
        rows = jnp.concatenate([x_seq, b_seq, c_seq], axis=1)
        act = conv_silu(jnp.pad(rows, ((CONV_K - 1, 0), (0, 0))), taps, LENGTH)
        xs = act[:, :INNER].reshape(LENGTH, HEADS, HEAD_DIM)
        bm = jnp.repeat(act[:, INNER:INNER + span].reshape(LENGTH, GROUPS, STATE), per_group, axis=1)
        cm = jnp.repeat(act[:, INNER + span:].reshape(LENGTH, GROUPS, STATE), per_group, axis=1)
        step = jax.nn.softplus(s_seq.astype(jnp.float32) + step_bias[None, :])
        y, _ = block_scan(xs, step, rate, bm, cm, BLOCK, jnp.zeros((HEADS, HEAD_DIM, STATE), jnp.float32))
        scanned = (y + skip[None, :, None] * xs).reshape(LENGTH, INNER).astype(jnp.bfloat16)
        gated = (scanned.astype(jnp.float32) * jax.nn.silu(g_seq.astype(jnp.float32))).reshape(LENGTH, GROUPS, INNER // GROUPS)
        gated = gated * lax.rsqrt(lax.optimization_barrier(jnp.mean(gated * gated, axis=2, keepdims=True)) + EPS)
        normed = (gated.reshape(LENGTH, INNER) * norm_gain[None, :]).astype(jnp.bfloat16)
        mixed = (r_seq.astype(jnp.float32) + jnp.dot(normed, out_weight, preferred_element_type=jnp.float32)).astype(jnp.bfloat16)
        mixed_f = mixed.astype(jnp.float32)
        expert_in = (mixed_f * lax.rsqrt(lax.optimization_barrier(jnp.mean(mixed_f * mixed_f, axis=1, keepdims=True)) + EPS) * ffn_gain[None, :]).astype(jnp.bfloat16)
        shared_hidden = (jax.nn.silu(jnp.dot(expert_in, shared_gate, preferred_element_type=jnp.float32)) * jnp.dot(expert_in, shared_up, preferred_element_type=jnp.float32)).astype(jnp.bfloat16)
        base = mixed_f + jnp.dot(shared_hidden, shared_down, preferred_element_type=jnp.float32)
        return (base, expert_in)
    base, expert_in = lax.map(one_sequence, (head_input, b_input, c_input, step_input, gate_input, residual))
    rows_all = SEQS * LENGTH
    flat_in = expert_in.reshape(rows_all, D)
    chosen = routes.reshape(-1).astype(jnp.int32)
    pairs = chosen.shape[0]
    onehot = (chosen[:, None] == jnp.arange(EXPERTS, dtype=jnp.int32)[None, :]).astype(jnp.int32)
    rank = lax.optimization_barrier(jnp.sum((jnp.cumsum(onehot, axis=0) - onehot) * onehot, axis=1)).astype(jnp.int32)
    room = N_SP * N_DP * CAP
    table = jnp.full((EXPERTS, room), pairs, jnp.int32).at[chosen, rank].set(jnp.arange(pairs, dtype=jnp.int32))

    def serve(carry, item):
        index, gate_w, up_w, down_w = item
        rows = jnp.take(flat_in, jnp.minimum(index, pairs - 1) // TOP_K, axis=0)
        hidden = (jax.nn.silu(jnp.dot(rows, gate_w, preferred_element_type=jnp.float32)) * jnp.dot(rows, up_w, preferred_element_type=jnp.float32)).astype(jnp.bfloat16)
        done = jnp.dot(hidden, down_w, preferred_element_type=jnp.float32).astype(jnp.bfloat16)
        return (carry.at[index].set(done, mode='drop'), None)
    pair_out, _ = lax.scan(serve, jnp.zeros((pairs, D), jnp.bfloat16), (table, expert_gate, expert_up, expert_down))
    routed = lax.optimization_barrier(jnp.sum(pair_out.reshape(rows_all, TOP_K, D).astype(jnp.float32) * route_weights.reshape(rows_all, TOP_K, 1), axis=1))
    return (base.reshape(rows_all, D) + routed).astype(jnp.bfloat16).reshape(SEQS, LENGTH, D)
```

```python
import jax
import jax.numpy as jnp
from jax import lax
from jax.experimental import pallas as pl
from jax.experimental.pallas import tpu as pltpu
from jax.sharding import PartitionSpec as P

EPS = 1e-06
HIGH = lax.Precision.HIGHEST
HALO = 8
F32 = jnp.float32
BF16 = jnp.bfloat16


def silu(v):
    return v * (1.0 / (1.0 + jnp.exp(-v)))


def conv_silu(halo, rows, taps):
    count = taps.shape[0]
    length = rows.shape[0]
    padded = jnp.concatenate([halo.astype(F32), rows.astype(F32)], axis=0)
    total = None
    for tap in range(count):
        start = HALO - (count - 1) + tap
        term = padded[start : start + length] * taps[tap : tap + 1].astype(F32)
        total = term if total is None else total + term
    return silu(total)


def spread(columns, first, count, width):
    rows = columns.shape[0]
    return jnp.concatenate(
        [jnp.broadcast_to(columns[:, first + j : first + j + 1], (rows, width)) for j in range(count)],
        axis=1,
    )


def block_kernel(
    x_ref, b_ref, c_ref, halo_ref, step_ref, wx_ref, wb_ref, wc_ref, bias_ref, log_ref, skip_ref,
    y_ref, cm_ref, grow_ref, state_ref, *, groups,
):
    length, inner = x_ref.shape
    heads = step_ref.shape[1]
    span = b_ref.shape[1]
    per = heads // groups
    width = inner // heads
    state = span // groups
    wide = per * width
    raw = step_ref[...].astype(F32) + bias_ref[...]
    step = jnp.maximum(raw, 0.0) + jnp.log(1.0 + jnp.exp(-jnp.abs(raw)))
    logs = step * -jnp.exp(log_ref[...])
    row = lax.broadcasted_iota(jnp.int32, (length, length), 0)
    col = lax.broadcasted_iota(jnp.int32, (length, length), 1)
    lower = row >= col
    tril = lower.astype(F32)
    cum = lax.dot_general(tril, logs, (((1,), (0,)), ((), ())), precision=HIGH, preferred_element_type=F32)
    cum_t = lax.dot_general(logs, tril, (((0,), (1,)), ((), ())), precision=HIGH, preferred_element_type=F32)
    grow_ref[...] = cum
    to_end = jnp.exp(cum[length - 1 : length] - cum)
    for g in range(groups):
        xcol = slice(g * wide, (g + 1) * wide)
        bcol = slice(g * state, (g + 1) * state)
        xs = conv_silu(halo_ref[:, xcol], x_ref[:, xcol], wx_ref[:, xcol])
        bm = conv_silu(
            halo_ref[:, inner + g * state : inner + (g + 1) * state], b_ref[:, bcol], wb_ref[:, bcol]
        ).astype(BF16)
        cm = conv_silu(
            halo_ref[:, inner + span + g * state : inner + span + (g + 1) * state],
            c_ref[:, bcol], wc_ref[:, bcol],
        ).astype(BF16)
        cm_ref[:, bcol] = cm
        weighted = xs * spread(step, g * per, per, width)
        scores = lax.dot_general(cm, bm, (((1,), (1,)), ((), ())), preferred_element_type=F32)
        scores = jnp.where(lower, scores, 0.0)
        parts = []
        small = weighted.astype(BF16)
        for j in range(per):
            h = g * per + j
            decay = jnp.exp(jnp.minimum(cum[:, h : h + 1] - cum_t[h : h + 1, :], 0.0))
            parts.append(
                jnp.dot((scores * decay).astype(BF16), small[:, j * width : (j + 1) * width],
                        preferred_element_type=F32)
            )
        y_ref[:, xcol] = jnp.concatenate(parts, axis=1) + skip_ref[:, xcol] * xs
        ended = (weighted * spread(to_end, g * per, per, width)).astype(BF16)
        state_ref[xcol, :] = lax.dot_general(
            ended, bm, (((0,), (0,)), ((), ())), preferred_element_type=F32
        ).astype(BF16)


def norm_kernel(y_ref, cm_ref, grow_ref, before_ref, gate_ref, gain_ref, out_ref, *, groups):
    length, inner = y_ref.shape
    heads = grow_ref.shape[1]
    state = before_ref.shape[1]
    per = heads // groups
    width = inner // heads
    wide = per * width
    grow = jnp.exp(grow_ref[...])
    for g in range(groups):
        xcol = slice(g * wide, (g + 1) * wide)
        outer = lax.dot_general(
            cm_ref[:, g * state : (g + 1) * state], before_ref[xcol, :],
            (((1,), (1,)), ((), ())), preferred_element_type=F32,
        )
        v = y_ref[:, xcol] + outer * spread(grow, g * per, per, width)
        v = v * silu(gate_ref[:, xcol].astype(F32))
        v = v * lax.rsqrt(jnp.mean(v * v, axis=1, keepdims=True) + EPS)
        out_ref[:, xcol] = (v * gain_ref[:, xcol]).astype(BF16)


def vmem(count):
    return [pl.BlockSpec(memory_space=pltpu.VMEM)] * count


PARAMS = pltpu.CompilerParams(vmem_limit_bytes=32 * 1024 * 1024)


def body(
    residual, head_input, gate_input, b_input, c_input, step_input, conv_weight, conv_b_weight,
    conv_c_weight, step_bias, decay_log, skip, norm_gain, out_weight, ffn_gain, shared_gate,
    shared_up, shared_down, expert_gate, expert_up, expert_down, routes, route_weights,
):
    tokens, inner = head_input.shape[1:]
    heads = step_bias.shape[0]
    state = 128
    span = b_input.shape[2]
    groups = span // state
    width = inner // heads
    model = residual.shape[2]
    ways = lax.axis_size("sp")
    place = lax.axis_index("sp")
    local = heads // ways
    x_rows, b_rows, c_rows = head_input[0], b_input[0], c_input[0]
    weight = lax.all_gather(out_weight, "dp", axis=0, tiled=True)
    tail = jnp.concatenate([x_rows[-HALO:], b_rows[-HALO:], c_rows[-HALO:]], axis=1)
    halo = lax.ppermute(tail, "sp", [(i, i + 1) for i in range(ways - 1)])
    y, cm, cum, states = pl.pallas_call(
        lambda *refs: block_kernel(*refs, groups=groups),
        out_shape=(
            jax.ShapeDtypeStruct((tokens, inner), F32),
            jax.ShapeDtypeStruct((tokens, span), BF16),
            jax.ShapeDtypeStruct((tokens, heads), F32),
            jax.ShapeDtypeStruct((inner, state), BF16),
        ),
        in_specs=vmem(11),
        out_specs=tuple(vmem(4)),
        compiler_params=PARAMS,
        cost_estimate=pl.CostEstimate(flops=400_000_000, bytes_accessed=5_000_000, transcendentals=1_500_000),
    )(
        x_rows, b_rows, c_rows, halo, step_input[0], conv_weight, conv_b_weight, conv_c_weight,
        step_bias[None], decay_log[None], jnp.repeat(skip, width)[None],
    )
    totals = lax.all_gather(cum[-1:], "sp", axis=0, tiled=True)
    arrived = lax.all_to_all(
        states.reshape(ways, local * width, state), "sp", split_axis=0, concat_axis=0, tiled=True
    )
    factors = jnp.repeat(
        jnp.exp(lax.dynamic_slice_in_dim(totals, place * local, local, 1)), width, axis=1
    )[:, :, None]
    carry = jnp.zeros((local * width, state), F32)
    prefix = []
    for i in range(ways):
        prefix.append(carry.astype(BF16))
        carry = carry * factors[i] + arrived[i].astype(F32)
    before = lax.all_to_all(jnp.stack(prefix), "sp", split_axis=0, concat_axis=0, tiled=True).reshape(
        inner, state
    )
    normed = pl.pallas_call(
        lambda *refs: norm_kernel(*refs, groups=groups),
        out_shape=jax.ShapeDtypeStruct((tokens, inner), BF16),
        in_specs=vmem(6),
        out_specs=vmem(1)[0],
        compiler_params=PARAMS,
        cost_estimate=pl.CostEstimate(flops=100_000_000, bytes_accessed=3_000_000, transcendentals=400_000),
    )(y, cm, cum, before, gate_input[0], norm_gain[None])

    mixed = (residual[0].astype(F32) + jnp.dot(normed, weight, preferred_element_type=F32)).astype(BF16)
    mixed_f = mixed.astype(F32)
    expert_in = (
        mixed_f * lax.rsqrt(jnp.mean(mixed_f * mixed_f, axis=1, keepdims=True) + EPS) * ffn_gain[None, :]
    ).astype(BF16)

    picks = routes.shape[2]
    ranks = ways * lax.axis_size("dp")
    experts = ranks * expert_gate.shape[0]
    slots = 2 * tokens * picks // experts
    chosen = routes[0].reshape(-1)
    pairs = chosen.shape[0]
    onehot = (chosen[:, None] == jnp.arange(experts, dtype=jnp.int32)[None, :]).astype(BF16)
    earlier = (jnp.arange(pairs)[:, None] > jnp.arange(pairs)[None, :]).astype(BF16)
    counts = jnp.dot(earlier, onehot, preferred_element_type=F32)
    position = jnp.sum(counts * onehot.astype(F32), axis=1).astype(jnp.int32)
    target = (chosen * slots + position).reshape(tokens, picks)
    lanes = jnp.arange(experts * slots, dtype=jnp.int32)
    combine = jnp.zeros((tokens, experts * slots), F32)
    choose = jnp.zeros((experts * slots, tokens), BF16)
    for k in range(picks):
        combine = combine + jnp.where(target[:, k, None] == lanes[None, :], route_weights[0][:, k, None], 0.0)
        choose = choose + (lanes[:, None] == target[None, :, k]).astype(BF16)
    high = combine.astype(BF16)
    low = (combine - high.astype(F32)).astype(BF16)

    outgoing = jnp.dot(choose, expert_in, preferred_element_type=F32).astype(BF16)
    got = lax.all_to_all(
        outgoing.reshape(experts, slots, model), ("sp", "dp"), split_axis=0, concat_axis=0, tiled=True
    )
    own = expert_gate.shape[0]
    shaped = got.reshape(ranks, own, slots, model)
    if own == 1:
        flat = got.reshape(ranks * slots, model)
        gate = jnp.dot(flat, expert_gate[0], preferred_element_type=F32)
        up = jnp.dot(flat, expert_up[0], preferred_element_type=F32)
        hidden = (jax.nn.silu(gate) * up).astype(BF16)
        done = jnp.dot(hidden, expert_down[0], preferred_element_type=F32).astype(BF16)
    else:
        gate = jnp.einsum("aenc,ecf->aenf", shaped, expert_gate, preferred_element_type=F32)
        up = jnp.einsum("aenc,ecf->aenf", shaped, expert_up, preferred_element_type=F32)
        hidden = (jax.nn.silu(gate) * up).astype(BF16)
        done = jnp.einsum("aenf,efc->aenc", hidden, expert_down, preferred_element_type=F32).astype(BF16)
    returned = lax.all_to_all(
        done.reshape(experts, slots, model), ("sp", "dp"), split_axis=0, concat_axis=0, tiled=True
    ).reshape(experts * slots, model)
    shared_hidden = (
        jax.nn.silu(jnp.dot(expert_in, shared_gate, preferred_element_type=F32))
        * jnp.dot(expert_in, shared_up, preferred_element_type=F32)
    ).astype(BF16)
    shared = mixed_f + jnp.dot(shared_hidden, shared_down, preferred_element_type=F32)
    routed = jnp.dot(high, returned, preferred_element_type=F32) + jnp.dot(
        low, returned, preferred_element_type=F32
    )
    return (shared + routed).astype(BF16)[None]


def solution(mesh):
    rows = P("dp", "sp", None)
    split = P(("sp", "dp"), None, None)
    return jax.shard_map(
        body,
        mesh=mesh,
        in_specs=(rows,) * 6 + (P(),) * 7 + (P("dp", None),) + (P(),) * 4 + (split,) * 3 + (rows,) * 2,
        out_specs=rows,
        check_vma=False,
    )
```

```python
import jax
import jax.numpy as jnp
from jax import lax
from jax.experimental import pallas as pl
from jax.experimental.pallas import tpu as pltpu
from jax.sharding import PartitionSpec as P

EPS = 1e-06
HIGH = lax.Precision.HIGHEST
HALO = 8
TAIL = 16
F32 = jnp.float32
BF16 = jnp.bfloat16


def silu(v):
    return v * (1.0 / (1.0 + jnp.exp(-v)))


def conv_silu(halo, rows, taps):
    count = taps.shape[0]
    length = rows.shape[0]
    padded = jnp.concatenate([halo.astype(F32), rows.astype(F32)], axis=0)
    total = None
    for tap in range(count):
        start = HALO - (count - 1) + tap
        term = padded[start : start + length] * taps[tap : tap + 1].astype(F32)
        total = term if total is None else total + term
    return silu(total)


def spread(columns, first, count, width):
    rows = columns.shape[0]
    return jnp.concatenate(
        [jnp.broadcast_to(columns[:, first + j : first + j + 1], (rows, width)) for j in range(count)],
        axis=1,
    )


def block_kernel(
    x_ref, b_ref, c_ref, halo_ref, step_ref, wx_ref, wb_ref, wc_ref, bias_ref, log_ref, skip_ref,
    y_ref, cm_ref, grow_ref, state_ref, *, groups, local,
):
    length, inner = x_ref.shape
    heads = step_ref.shape[1]
    span = b_ref.shape[1]
    per = heads // groups
    width = inner // heads
    state = span // groups
    wide = per * width
    raw = step_ref[...].astype(F32) + bias_ref[...]
    step = jnp.maximum(raw, 0.0) + jnp.log(1.0 + jnp.exp(-jnp.abs(raw)))
    logs = step * -jnp.exp(log_ref[...])
    row = lax.broadcasted_iota(jnp.int32, (length, length), 0)
    col = lax.broadcasted_iota(jnp.int32, (length, length), 1)
    lower = row >= col
    tril = lower.astype(F32)
    cum = lax.dot_general(tril, logs, (((1,), (0,)), ((), ())), precision=HIGH, preferred_element_type=F32)
    cum_t = lax.dot_general(logs, tril, (((0,), (1,)), ((), ())), precision=HIGH, preferred_element_type=F32)
    grow_ref[...] = cum
    to_end = jnp.exp(cum[length - 1 : length] - cum)
    for g in range(groups):
        xcol = slice(g * wide, (g + 1) * wide)
        bcol = slice(g * state, (g + 1) * state)
        xs = conv_silu(halo_ref[:, xcol], x_ref[:, xcol], wx_ref[:, xcol])
        bm = conv_silu(
            halo_ref[:, inner + g * state : inner + (g + 1) * state], b_ref[:, bcol], wb_ref[:, bcol]
        ).astype(BF16)
        cm = conv_silu(
            halo_ref[:, inner + span + g * state : inner + span + (g + 1) * state],
            c_ref[:, bcol], wc_ref[:, bcol],
        ).astype(BF16)
        cm_ref[:, bcol] = cm
        weighted = xs * spread(step, g * per, per, width)
        scores = lax.dot_general(cm, bm, (((1,), (1,)), ((), ())), preferred_element_type=F32)
        scores = jnp.where(lower, scores, 0.0)
        parts = []
        small = weighted.astype(BF16)
        for j in range(per):
            h = g * per + j
            decay = jnp.exp(jnp.minimum(cum[:, h : h + 1] - cum_t[h : h + 1, :], 0.0))
            parts.append(
                jnp.dot((scores * decay).astype(BF16), small[:, j * width : (j + 1) * width],
                        preferred_element_type=F32)
            )
        y_ref[:, xcol] = jnp.concatenate(parts, axis=1) + skip_ref[:, xcol] * xs
        ended = (weighted * spread(to_end, g * per, per, width)).astype(BF16)
        fresh = lax.dot_general(
            ended, bm, (((0,), (0,)), ((), ())), preferred_element_type=F32
        ).astype(BF16)
        for j in range(per):
            h = g * per + j
            at = h % local * width
            state_ref[h // local, at : at + width, :] = fresh[j * width : (j + 1) * width]
    last = cum[length - 1 : length]
    high = last.astype(BF16)
    rest = last - high.astype(F32)
    middle = rest.astype(BF16)
    low = (rest - middle.astype(F32)).astype(BF16)
    for w in range(heads // local):
        mine = slice(w * local, (w + 1) * local)
        parts = [p.astype(F32)[:, mine] for p in (high, middle, low)]
        rows = jnp.concatenate(parts + [jnp.zeros((TAIL - 3, local), F32)], axis=0)
        rows = jnp.concatenate([rows, jnp.zeros((TAIL, state - local), F32)], axis=1)
        state_ref[w, local * width :, :] = rows.astype(BF16)


def prefix_kernel(got_ref, out_ref, *, local):
    ways, rows, state = out_ref.shape
    width = rows // local
    factors = []
    for i in range(ways - 1):
        tail = got_ref[i, rows : rows + TAIL, :].astype(F32)
        factors.append(jnp.exp(tail[0:1] + tail[1:2] + tail[2:3]))
    for j in range(local):
        at = slice(j * width, (j + 1) * width)
        carry = jnp.zeros((width, state), F32)
        for i in range(ways):
            out_ref[i, at, :] = carry.astype(BF16)
            if i < ways - 1:
                factor = jnp.broadcast_to(factors[i][:, j : j + 1], (1, state))
                carry = carry * factor + got_ref[i, at, :].astype(F32)


def norm_kernel(y_ref, cm_ref, grow_ref, before_ref, gate_ref, gain_ref, out_ref, *, groups):
    length, inner = y_ref.shape
    heads = grow_ref.shape[1]
    state = before_ref.shape[1]
    per = heads // groups
    width = inner // heads
    wide = per * width
    grow = jnp.exp(grow_ref[...])
    for g in range(groups):
        xcol = slice(g * wide, (g + 1) * wide)
        outer = lax.dot_general(
            cm_ref[:, g * state : (g + 1) * state], before_ref[xcol, :],
            (((1,), (1,)), ((), ())), preferred_element_type=F32,
        )
        v = y_ref[:, xcol] + outer * spread(grow, g * per, per, width)
        v = v * silu(gate_ref[:, xcol].astype(F32))
        v = v * lax.rsqrt(jnp.mean(v * v, axis=1, keepdims=True) + EPS)
        out_ref[:, xcol] = (v * gain_ref[:, xcol]).astype(BF16)


def vmem(count):
    return [pl.BlockSpec(memory_space=pltpu.VMEM)] * count


PARAMS = pltpu.CompilerParams(vmem_limit_bytes=32 * 1024 * 1024)


def body(
    residual, head_input, gate_input, b_input, c_input, step_input, conv_weight, conv_b_weight,
    conv_c_weight, step_bias, decay_log, skip, norm_gain, out_weight, ffn_gain, shared_gate,
    shared_up, shared_down, expert_gate, expert_up, expert_down, routes, route_weights,
):
    tokens, inner = head_input.shape[1:]
    heads = step_bias.shape[0]
    state = 128
    span = b_input.shape[2]
    groups = span // state
    width = inner // heads
    model = residual.shape[2]
    ways = lax.axis_size("sp")
    local = heads // ways
    x_rows, b_rows, c_rows = head_input[0], b_input[0], c_input[0]
    weight = lax.all_gather(out_weight, "dp", axis=0, tiled=True)
    tail = jnp.concatenate([x_rows[-HALO:], b_rows[-HALO:], c_rows[-HALO:]], axis=1)
    halo = lax.ppermute(tail, "sp", [(i, i + 1) for i in range(ways - 1)])
    y, cm, cum, states = pl.pallas_call(
        lambda *refs: block_kernel(*refs, groups=groups, local=local),
        out_shape=(
            jax.ShapeDtypeStruct((tokens, inner), F32),
            jax.ShapeDtypeStruct((tokens, span), BF16),
            jax.ShapeDtypeStruct((tokens, heads), F32),
            jax.ShapeDtypeStruct((ways, local * width + TAIL, state), BF16),
        ),
        in_specs=vmem(11),
        out_specs=tuple(vmem(4)),
        compiler_params=PARAMS,
        cost_estimate=pl.CostEstimate(flops=400_000_000, bytes_accessed=5_000_000, transcendentals=1_500_000),
    )(
        x_rows, b_rows, c_rows, halo, step_input[0], conv_weight, conv_b_weight, conv_c_weight,
        step_bias[None], decay_log[None], jnp.repeat(skip, width)[None],
    )
    arrived = lax.all_to_all(states, "sp", split_axis=0, concat_axis=0, tiled=True)
    prefix = pl.pallas_call(
        lambda *refs: prefix_kernel(*refs, local=local),
        out_shape=jax.ShapeDtypeStruct((ways, local * width, state), BF16),
        in_specs=vmem(1),
        out_specs=vmem(1)[0],
        compiler_params=PARAMS,
        cost_estimate=pl.CostEstimate(flops=2_000_000, bytes_accessed=1_000_000, transcendentals=1000),
    )(arrived)
    before = lax.all_to_all(prefix, "sp", split_axis=0, concat_axis=0, tiled=True).reshape(inner, state)
    normed = pl.pallas_call(
        lambda *refs: norm_kernel(*refs, groups=groups),
        out_shape=jax.ShapeDtypeStruct((tokens, inner), BF16),
        in_specs=vmem(6),
        out_specs=vmem(1)[0],
        compiler_params=PARAMS,
        cost_estimate=pl.CostEstimate(flops=100_000_000, bytes_accessed=3_000_000, transcendentals=400_000),
    )(y, cm, cum, before, gate_input[0], norm_gain[None])

    mixed = (residual[0].astype(F32) + jnp.dot(normed, weight, preferred_element_type=F32)).astype(BF16)
    mixed_f = mixed.astype(F32)
    expert_in = (
        mixed_f * lax.rsqrt(jnp.mean(mixed_f * mixed_f, axis=1, keepdims=True) + EPS) * ffn_gain[None, :]
    ).astype(BF16)

    picks = routes.shape[2]
    ranks = ways * lax.axis_size("dp")
    experts = ranks * expert_gate.shape[0]
    slots = 2 * tokens * picks // experts
    chosen = routes[0].reshape(-1)
    pairs = chosen.shape[0]
    onehot = (chosen[:, None] == jnp.arange(experts, dtype=jnp.int32)[None, :]).astype(BF16)
    earlier = (jnp.arange(pairs)[:, None] > jnp.arange(pairs)[None, :]).astype(BF16)
    counts = jnp.dot(earlier, onehot, preferred_element_type=F32)
    position = jnp.sum(counts * onehot.astype(F32), axis=1).astype(jnp.int32)
    target = (chosen * slots + position).reshape(tokens, picks)
    lanes = jnp.arange(experts * slots, dtype=jnp.int32)
    combine = jnp.zeros((tokens, experts * slots), F32)
    choose = jnp.zeros((experts * slots, tokens), BF16)
    for k in range(picks):
        combine = combine + jnp.where(target[:, k, None] == lanes[None, :], route_weights[0][:, k, None], 0.0)
        choose = choose + (lanes[:, None] == target[None, :, k]).astype(BF16)
    high = combine.astype(BF16)
    low = (combine - high.astype(F32)).astype(BF16)

    outgoing = jnp.dot(choose, expert_in, preferred_element_type=F32).astype(BF16)
    got = lax.all_to_all(
        outgoing.reshape(experts, slots, model), ("sp", "dp"), split_axis=0, concat_axis=0, tiled=True
    )
    own = expert_gate.shape[0]
    shaped = got.reshape(ranks, own, slots, model)
    if own == 1:
        flat = got.reshape(ranks * slots, model)
        gate = jnp.dot(flat, expert_gate[0], preferred_element_type=F32)
        up = jnp.dot(flat, expert_up[0], preferred_element_type=F32)
        hidden = (jax.nn.silu(gate) * up).astype(BF16)
        done = jnp.dot(hidden, expert_down[0], preferred_element_type=F32).astype(BF16)
    else:
        gate = jnp.einsum("aenc,ecf->aenf", shaped, expert_gate, preferred_element_type=F32)
        up = jnp.einsum("aenc,ecf->aenf", shaped, expert_up, preferred_element_type=F32)
        hidden = (jax.nn.silu(gate) * up).astype(BF16)
        done = jnp.einsum("aenf,efc->aenc", hidden, expert_down, preferred_element_type=F32).astype(BF16)
    returned = lax.all_to_all(
        done.reshape(experts, slots, model), ("sp", "dp"), split_axis=0, concat_axis=0, tiled=True
    ).reshape(experts * slots, model)
    shared_hidden = (
        jax.nn.silu(jnp.dot(expert_in, shared_gate, preferred_element_type=F32))
        * jnp.dot(expert_in, shared_up, preferred_element_type=F32)
    ).astype(BF16)
    shared = mixed_f + jnp.dot(shared_hidden, shared_down, preferred_element_type=F32)
    routed = jnp.dot(high, returned, preferred_element_type=F32) + jnp.dot(
        low, returned, preferred_element_type=F32
    )
    return (shared + routed).astype(BF16)[None]


def solution(mesh):
    rows = P("dp", "sp", None)
    split = P(("sp", "dp"), None, None)
    return jax.shard_map(
        body,
        mesh=mesh,
        in_specs=(rows,) * 6 + (P(),) * 7 + (P("dp", None),) + (P(),) * 4 + (split,) * 3 + (rows,) * 2,
        out_specs=rows,
        check_vma=False,
    )
```
